32 devices in a mesh: sp: 8 (over z, y), tp: 4 (over x, core).
Axes of the slice: x: 2, y: 2, z: 4, core: 2. Of those that a mesh axis runs over, the one named last changes fastest.
Arguments:
- residual: bfloat16 [4, 768, 2048], P('tp', 'sp'), may hold values from -3 to 3
- query_nope: bfloat16 [4, 768, 1024], P('tp', 'sp'), may hold values from -9 to 9
- query_rope: bfloat16 [4, 768, 512], P('tp', 'sp'), may hold values from -48 to 48
- latent: bfloat16 [4, 768, 128], P('tp', 'sp'), may hold values from -6 to 6
- rope_key: bfloat16 [4, 768, 32], P('tp', 'sp'), may hold values from -48 to 48
- latent_gain: float32 [128], replicated, may hold values from 0.1 to 1.9
- up_key: bfloat16 [128, 1024], replicated, may hold values from -1 to 1
- up_value: bfloat16 [128, 1024], replicated, may hold values from -0.5 to 0.5
- out_weight: bfloat16 [1024, 2048], replicated, may hold values from -0.375 to 0.375
- ffn_gain: float32 [2048], replicated, may hold values from 0.1 to 1.9
- routes: int32 [4, 768, 2], P(None, 'sp'), may hold values from 0 to 7, all different within a row; in each aligned block of 96 rows (0 to 95, 96 to 191, ..., all dimensions but the last counted through in order) at most 30 rows name the same one
- route_weight: float32 [4, 768, 2], P('tp', 'sp'), may hold values from 0.1 to 1
- gate_weight: bfloat16 [8, 2048, 1024], P('sp', None, 'tp'), may hold values from -1.5 to 1.5
- up_weight: bfloat16 [8, 2048, 1024], P('sp', None, 'tp'), may hold values from -1.5 to 1.5
- down_weight: bfloat16 [8, 1024, 2048], P('sp', 'tp'), may hold values from -0.046875 to 0.046875
Outputs:
- updated: bfloat16 [4, 768, 2048], P('tp', 'sp')
The draws below stay inside these ranges and needn't reach their ends.
Inputs may be any that keep to these rules, and one draw needn't show every extreme that they name: `routes`: each row names 2 different experts. In each aligned block of 96 rows (one sequence's rows of one device) no expert is named by more than 30 rows, a bound that some block reaches.
All inputs are finite; a program needn't handle non-finite values.
Results may differ from the reference program's by a relative error of at most 0.017.
Values may be sent and summed in bfloat16 or wider, within the bound.
A program may use at most 64 MiB of HBM per device.

```python
import math
import jax
import jax.numpy as jnp
import numpy as np
from jax import lax

D = 2048
HEADS = 16
NOPE = 64
ROPE = 32
VDIM = 64
LATENT = 128
FF = 1024
TOPK = 2
TOK_DEV = 96
SEQS = 4
LENGTH = 768
EXPERTS = 8
FF_BLOCK = 256
MOST = 30
N_SP = 8
N_TP = 4


def rope_pair(key):
    base = jax.random.fold_in(key, 7)
    shape_keys = (SEQS, LENGTH, ROPE)
    shape_queries = (SEQS, LENGTH, HEADS, ROPE)
    keys = jax.random.normal(jax.random.fold_in(base, 1), shape_keys, jnp.float32) * 1.5
    queries = jax.random.normal(jax.random.fold_in(base, 2), shape_queries, jnp.float32) * 1.5
    return (keys, queries.reshape(SEQS, LENGTH, HEADS * ROPE))


def expert_matrix(key, salt):
    base = jax.random.fold_in(key, salt)
    values = jax.random.normal(jax.random.fold_in(base, 1), (EXPERTS, D, FF), jnp.float32)
    columns = jnp.exp(jax.random.uniform(jax.random.fold_in(base, 2), (EXPERTS, 1, FF), jnp.float32, math.log(0.5), math.log(6.0)))
    return jnp.clip(values * columns * D ** (-0.5), -1.5, 1.5)


def draw_query_rope(key, part):
    return rope_pair(key)[1].astype(jnp.bfloat16)


def draw_rope_key(key, part):
    return rope_pair(key)[0].astype(jnp.bfloat16)


def draw_gate_weight(key, part):
    return expert_matrix(key, 101).astype(jnp.bfloat16)


def draw_up_weight(key, part):
    return expert_matrix(key, 202).astype(jnp.bfloat16)


def level_of(stream_key, shape, shards, low, high):
    level, own = 1.0, jax.random.fold_in(stream_key, 6)
    for dim, shards_of in shards:
        steps = jnp.exp(jax.random.uniform(jax.random.fold_in(own, dim), (shards_of,), jnp.float32, low / len(shards), high / len(shards)))
        level = level * jnp.repeat(steps, shape[dim] // shards_of).reshape([-1 if axis == dim else 1 for axis in range(len(shape))])
    return level


def shared_out(own_key, own, number, rows, amount, top, limit, lean):
    order = jax.random.permutation(own_key, amount)
    packed, ordinary = load_shares(amount, rows * top, limit, lean, True), load_shares(amount, rows * top, limit, lean, False)
    places = jnp.arange(amount)

    def named(tallies, offset_by):
        used = int((tallies > 0).sum())
        fixed = max(1, used // 4)
        passed = fixed + (places - fixed + offset_by * (used - fixed)) % max(1, amount - fixed)
        return jnp.zeros((amount,), jnp.int32).at[order[jnp.where(places < fixed, places, passed)]].set(jnp.asarray(tallies, jnp.int32))

    tallies = jnp.where(number % 4 == 0, named(packed, number // 4), named(ordinary, number - number // 4 - 1))
    mixed = jax.random.permutation(jax.random.fold_in(own, 3), amount)
    giver, sink = mixed[0:amount // 2 * 2:2], mixed[1:amount // 2 * 2:2]
    room = jnp.minimum(tallies[giver] - 1, limit - tallies[sink]) // 2
    room = jnp.where((giver == order[0]) | (sink == order[0]) | (tallies[sink] == 0), 0, jnp.maximum(room, 0))
    passed = jax.random.randint(jax.random.fold_in(own, 4), (amount // 2,), 0, 1 << 20) % (room + 1)
    tallies = tallies.at[giver].add(-passed).at[sink].add(passed)
    members = jnp.searchsorted(jnp.cumsum(tallies), jnp.arange(rows * top), side="right").astype(jnp.int32)
    grid = members.reshape(top, rows).T
    grid = grid[jax.random.permutation(jax.random.fold_in(own, 1), rows)]
    offset_by = jax.random.randint(jax.random.fold_in(own, 2), (rows, 1), 0, top)
    return jnp.take_along_axis(grid, (jnp.arange(top)[None, :] + offset_by) % top, axis=1)


def load_shares(count, total, reach, skew, full):
    portions = [(1 << 20) // math.isqrt(standing ** skew) + 1 for standing in range(1, count + 1)]
    largest = reach if full else min(reach, max(-(-total // count), total * portions[0] // sum(portions)))
    least = 1 if total - largest >= count - 1 else 0
    given, rest = [largest] + [least] * (count - 1), total - largest - least * (count - 1)
    while rest > 0:
        candidates = [i for i in range(1, count) if given[i] < largest] or [i for i in range(1, count) if given[i] < reach]
        whole, budget = sum([portions[i] for i in candidates]), rest
        for i in candidates:
            addition = min(reach - given[i], max(1, budget * portions[i] // whole), rest)
            given[i] = given[i] + addition
            rest = rest - addition
    return np.array(given)


def bell_draw(own_key, dims, spread, most, shards=(), held_as=jnp.bfloat16):
    loudness = level_of(own_key, dims, shards, -0.22, 0.18) if shards else 1.0
    values = jax.random.normal(own_key, dims, jnp.float32) * spread * loudness
    return jnp.minimum(jnp.maximum(values, -most), most).astype(held_as)


def setup_inputs(seed: int = 0) -> dict:
    key_list = jax.random.split(jax.random.key(seed), 16)
    residual = bell_draw(key_list[0], (SEQS, LENGTH, D), 0.5, 3.0, ((0, 4), (1, 8)))
    query_nope = bell_draw(key_list[1], (SEQS, LENGTH, HEADS * NOPE), 1.5, 9.0, ((0, 4), (1, 8)))
    query_rope = draw_query_rope(jax.random.fold_in(key_list[15], 71), 0)
    latent = bell_draw(key_list[3], (SEQS, LENGTH, LATENT), 1.0, 6.0, ((0, 4), (1, 8)))
    rope_key = draw_rope_key(jax.random.fold_in(key_list[15], 71), 0)
    latent_gain = jnp.clip(1.0 + 0.18 * jax.random.normal(key_list[5], (LATENT,), jnp.float32), 0.1, 1.9)
    up_key = bell_draw(key_list[6], (LATENT, HEADS * NOPE), (LATENT // 3) ** -0.5, 1.0)
    up_value = bell_draw(key_list[7], (LATENT, HEADS * VDIM), LATENT ** -0.5, 0.5)
    out_weight = bell_draw(key_list[8], (HEADS * VDIM, D), (HEADS * VDIM // 4) ** -0.5, 0.375)
    ffn_gain = jnp.clip(1.0 + 0.18 * jax.random.normal(key_list[9], (D,), jnp.float32), 0.1, 1.9)
    routes_keys = jax.random.split(jax.random.fold_in(key_list[10], 1), SEQS * LENGTH // TOK_DEV)
    routes_turns = jax.random.permutation(jax.random.fold_in(key_list[10], 3), SEQS * LENGTH // TOK_DEV)
    routes = jax.vmap(lambda own, number: shared_out(jax.random.fold_in(key_list[10], 2), own, number, TOK_DEV, EXPERTS, TOPK, MOST, 0))(routes_keys, routes_turns).reshape((SEQS, LENGTH, TOPK))
    route_weight = jnp.clip(jnp.exp(math.log(1.0) - 2.3025851 * jax.random.uniform(key_list[11], (SEQS, LENGTH, TOPK), jnp.float32) ** level_of(key_list[11], (SEQS, LENGTH, TOPK), ((0, 4), (1, 8)), -0.2, 0.2)), 0.1, 1.0)
    gate_weight = draw_gate_weight(jax.random.fold_in(key_list[15], 71), 0)
    up_weight = draw_up_weight(jax.random.fold_in(key_list[15], 71), 0)
    down_weight = bell_draw(key_list[14], (EXPERTS, FF, D), (FF * 16) ** -0.5, 0.046875, ((0, 8), (1, 4)))
    return dict(residual=residual, query_nope=query_nope, query_rope=query_rope, latent=latent, rope_key=rope_key, latent_gain=latent_gain, up_key=up_key, up_value=up_value, out_weight=out_weight, ffn_gain=ffn_gain, routes=routes, route_weight=route_weight, gate_weight=gate_weight, up_weight=up_weight, down_weight=down_weight)


EPS = 1e-06
ROPE_BASE = 10000.0
CLAMP = 7.0
ALPHA = 1.702

def rotate(values, positions, width):
    half = width // 2
    inverse = ROPE_BASE ** (-jnp.arange(half, dtype=jnp.float32) * 2.0 / width)
    angle = positions.astype(jnp.float32)[:, None] * inverse[None, :]
    cosine = jnp.cos(angle)[:, None, :]
    sine = jnp.sin(angle)[:, None, :]
    first = values[..., :half]
    second = values[..., half:]
    return jnp.concatenate([first * cosine - second * sine, first * sine + second * cosine], axis=-1)

def rms_scaled(values, gain):
    return values * lax.rsqrt(lax.optimization_barrier(jnp.mean(values * values, axis=-1, keepdims=True)) + EPS) * gain

def reference(residual, query_nope, query_rope, latent, rope_key, latent_gain, up_key, up_value, out_weight, ffn_gain, routes, route_weight, gate_weight, up_weight, down_weight):
    sequences, length, width = residual.shape
    positions = jnp.arange(length, dtype=jnp.int32)
    factor = (NOPE + ROPE) ** (-0.5)
    normed = rms_scaled(latent.astype(jnp.float32), latent_gain).astype(jnp.bfloat16)
    flat_latent = normed.reshape(-1, LATENT)
    key_part = jnp.dot(flat_latent, up_key, preferred_element_type=jnp.float32).astype(jnp.bfloat16)
    key_part = key_part.reshape(sequences, length, HEADS, NOPE)
    value_part = jnp.dot(flat_latent, up_value, preferred_element_type=jnp.float32).astype(jnp.bfloat16)
    value_part = value_part.reshape(sequences, length, HEADS, VDIM)
    key_turned = rotate(rope_key.astype(jnp.float32)[:, :, None, :], positions, ROPE)[:, :, 0, :].astype(jnp.bfloat16)
    query_turned = rotate(query_rope.astype(jnp.float32).reshape(sequences, length, HEADS, ROPE), positions, ROPE).astype(jnp.bfloat16)
    query_plain = query_nope.reshape(sequences, length, HEADS, NOPE)
    span = math.gcd(length, 256)
    count = length // span

    def one_sequence(items):
        plain, turned, keys, turned_keys, values = items
        keys_wide = keys.astype(jnp.float32)
        turned_wide = turned_keys.astype(jnp.float32)
        values_wide = values.astype(jnp.float32)

        def one_block(pair):
            scores = (jnp.einsum('qhd,khd->hqk', pair[0].astype(jnp.float32), keys_wide) + jnp.einsum('qhd,kd->hqk', pair[1].astype(jnp.float32), turned_wide)) * factor
            peak = lax.optimization_barrier(jnp.max(scores, axis=-1, keepdims=True))
            weights = jnp.exp(scores - peak)
            total = lax.optimization_barrier(jnp.sum(weights, axis=-1))
            rounded = lax.optimization_barrier(weights.astype(jnp.bfloat16)).astype(jnp.float32)
            mixed = jnp.einsum('hqk,khd->qhd', rounded, values_wide)
            return (mixed / jnp.transpose(total)[:, :, None]).astype(jnp.bfloat16)
        blocks = lax.map(one_block, (plain.reshape(count, span, HEADS, NOPE), turned.reshape(count, span, HEADS, ROPE)))
        return blocks.reshape(length, HEADS * VDIM)
    attended = lax.map(one_sequence, (query_plain, query_turned, key_part, key_turned, value_part))
    projected = jnp.dot(attended.reshape(-1, HEADS * VDIM), out_weight, preferred_element_type=jnp.float32)
    middle = (residual.reshape(-1, width).astype(jnp.float32) + projected).astype(jnp.bfloat16)
    middle_wide = lax.optimization_barrier(middle).astype(jnp.float32)
    normal_rows = rms_scaled(middle_wide, ffn_gain).astype(jnp.bfloat16)
    total_rows = sequences * length
    flat_picks = routes.reshape(-1)
    flat_weights = route_weight.reshape(-1)
    owner = jnp.arange(total_rows * TOPK, dtype=jnp.int32) // TOPK
    capacity = sequences * N_SP * MOST
    padded = jnp.concatenate([normal_rows, jnp.zeros((1, width), jnp.bfloat16)], axis=0)

    def one_expert(accum, items):
        gate_w, up_w, down_w, index = items
        hit = flat_picks == index
        rank = jnp.cumsum(hit.astype(jnp.int32)) - 1
        slot = jnp.where(hit, rank, capacity).astype(jnp.int32)
        source = jnp.full((capacity + 1,), total_rows, jnp.int32).at[slot].set(owner)[:capacity]
        scale_rows = jnp.zeros((capacity + 1,), jnp.float32).at[slot].set(flat_weights)[:capacity]
        rows = padded[source]
        gate = jnp.minimum(jnp.dot(rows, gate_w, preferred_element_type=jnp.float32), CLAMP)
        lift = jnp.clip(jnp.dot(rows, up_w, preferred_element_type=jnp.float32), -CLAMP, CLAMP)
        active = (gate * jax.nn.sigmoid(ALPHA * gate) * (lift + 1.0)).astype(jnp.bfloat16)
        parts = jnp.einsum('rjf,jfd->jrd', active.reshape(capacity, N_TP, FF_BLOCK).astype(jnp.float32), down_w.reshape(N_TP, FF_BLOCK, width).astype(jnp.float32))
        output = lax.optimization_barrier(jnp.sum(lax.optimization_barrier(parts.astype(jnp.bfloat16)).astype(jnp.float32), axis=0))
        output = output.astype(jnp.bfloat16)
        accum = accum.at[source].add(output.astype(jnp.float32) * scale_rows[:, None])
        return (accum, None)
    accum, _ = lax.scan(one_expert, jnp.zeros((total_rows + 1, width), jnp.float32), (gate_weight, up_weight, down_weight, jnp.arange(EXPERTS, dtype=jnp.int32)))
    updated = (middle_wide + accum[:total_rows]).astype(jnp.bfloat16)
    return updated.reshape(sequences, length, width)
```

```python
import functools

import jax
import jax.numpy as jnp
import numpy as np
from jax import lax
from jax.experimental import pallas as pl
from jax.experimental.pallas import tpu as pltpu
from jax.sharding import PartitionSpec as P

HEADS = 16
NOPE = 64
ROPE = 32
VDIM = 64
LATENT = 128
TOPK = 2
LANES = 128

EPS = 1e-06
ROPE_BASE = 10000.0
CLAMP = 7.0
ALPHA = 1.702
LOG2E = 1.4426950408889634
MESH = pl.DeviceIdType.MESH
VM = pl.BlockSpec(memory_space=pltpu.VMEM)
ANY = pl.BlockSpec(memory_space=pl.ANY)
F32 = jnp.float32
BF16 = jnp.bfloat16
BYCOL = (((1,), (1,)), ((), ()))


def swapped(x):
    lane = lax.broadcasted_iota(jnp.int32, x.shape, 1)
    half = ROPE // 2
    return jnp.where(
        lane % ROPE < half, pltpu.roll(x, x.shape[1] - half, 1), pltpu.roll(x, half, 1)
    )


def place(picks_ref, experts, slots, tokens):
    expert = lax.broadcasted_iota(jnp.int32, (experts, tokens), 0)
    hots = [(expert == picks_ref[k : k + 1, :]).astype(F32) for k in range(TOPK)]
    earlier = (
        lax.broadcasted_iota(jnp.int32, (tokens, tokens), 0)
        < lax.broadcasted_iota(jnp.int32, (tokens, tokens), 1)
    ).astype(F32)
    rank = jnp.dot(sum(hots), earlier, preferred_element_type=F32)
    where = rank + (expert * slots).astype(F32)
    slot = lax.broadcasted_iota(jnp.int32, (experts * slots, tokens), 0).astype(F32)
    return [
        (slot == jnp.sum(hot * where, axis=0, keepdims=True)).astype(F32) for hot in hots
    ]


def partners(me, d, n):
    if n & (n - 1):
        return lax.rem(me + d, n), lax.rem(me + n - d, n)
    peer, bit = me, 1
    while bit < n:
        if d & bit:
            peer = peer + bit * (1 - 2 * lax.rem(lax.div(me, bit), 2))
        bit *= 2
    return peer, peer


def layer_kernel(
    n, m, slots, parts,
    lat_any, rope_any, lgain_any, tab_any, qn_any, qr_any, upk_any, upv_any, ow_any, res_any,
    fgain_any, routes_any, share_any, gate_any, up_any, down_any,
    out_ref,
    lat_ref, rope_ref, lgain_ref, tab_ref, qn_ref, qr_ref, upk_ref, upv_ref, ow_ref, mid_ref,
    fgain_ref, picks_ref, share_ref, gu_ref, dw_ref,
    kv, keys, vals, query, att, norm, packer, high, low, sent, rows_a, rows_b, act, act_b, res, back,
    load_sem, send_sem, recv_sem,
):
    tokens, width = out_ref.shape
    hidden = gate_any.shape[1]
    groups = m // 2
    local = 2 * hidden
    me = lax.axis_index("sp")
    rank = lax.axis_index("tp")
    sibling = rank + 1 - 2 * lax.rem(rank, 2)
    count = n // parts
    span = count * slots
    step = 512
    order = list(range(n - 1, -1, -1))
    packed = tokens // (LANES // ROPE)

    barrier = pltpu.get_barrier_semaphore()
    for d in range(1, n):
        pl.semaphore_signal(
            barrier, inc=1, device_id={"sp": partners(me, d, n)[0]}, device_id_type=MESH
        )
    for j in range(1, groups):
        pl.semaphore_signal(
            barrier, inc=1, device_id={"tp": lax.rem(rank + 2 * j, m)}, device_id_type=MESH
        )
    pl.semaphore_signal(barrier, inc=1, device_id={"tp": sibling}, device_id_type=MESH)

    loads = {}

    def load(name, source, target):
        loads[name] = pltpu.make_async_copy(source, target, load_sem.at[len(loads)])
        loads[name].start()

    load("lat", lat_any, lat_ref)
    load("rope", rope_any, rope_ref)
    load("lgain", lgain_any, lgain_ref)
    load("tab", tab_any, tab_ref)
    load("qr", qr_any, qr_ref)
    load("qn", qn_any, qn_ref)
    load("upk", upk_any, upk_ref)
    load("picks", routes_any.at[rank], picks_ref)
    load("share", share_any, share_ref)
    load("upv", upv_any, upv_ref)
    load("ow", ow_any, ow_ref)
    load("res", res_any, mid_ref)
    load("fgain", fgain_any, fgain_ref)
    load("gate", gate_any, gu_ref.at[:, pl.ds(0, hidden)])
    load("up", up_any, gu_ref.at[:, pl.ds(local, hidden)])
    load("down", down_any, dw_ref.at[pl.ds(0, hidden)])

    used = [0]

    def remote(source, target, device):
        index = used[0]
        used[0] += 1
        copy = pltpu.make_async_remote_copy(
            src_ref=source,
            dst_ref=target,
            send_sem=send_sem.at[index],
            recv_sem=recv_sem.at[index],
            device_id=device,
            device_id_type=MESH,
        )
        copy.start()
        return copy

    for name in ("lat", "rope", "lgain", "tab"):
        loads[name].wait()
    base_cos = tab_ref[0, pl.ds(tokens + me, 1), :]
    base_sin = tab_ref[1, pl.ds(tokens + me, 1), :]
    cosine = tab_ref[0, :tokens, :] * base_cos - tab_ref[1, :tokens, :] * base_sin
    sine = tab_ref[1, :tokens, :] * base_cos + tab_ref[0, :tokens, :] * base_sin
    lat = lat_ref[...].astype(F32)
    mean = jnp.mean(lat * lat, axis=-1, keepdims=True)
    kv[0, :tokens, :] = (lat * lax.rsqrt(mean + EPS) * lgain_ref[...]).astype(BF16)
    wide = jnp.concatenate([rope_ref[...].astype(F32)] * (LANES // ROPE), axis=0)
    pad = -tokens % LANES
    if pad:
        wide = jnp.concatenate([wide, jnp.zeros((LANES, pad), F32)], axis=1)
    wide = jnp.transpose(wide)[:tokens]
    turned = wide * cosine + swapped(wide) * sine
    lane = lax.broadcasted_iota(jnp.int32, (packed, LANES), 1)
    masks = [(lane // ROPE == g).astype(F32) for g in range(LANES // ROPE)]
    strip = sum(turned[g * packed : (g + 1) * packed] * masks[g] for g in range(LANES // ROPE))
    rest = kv.shape[1] - tokens - packed
    if rest:
        strip = jnp.concatenate([strip, jnp.zeros((rest, LANES), F32)], axis=0)
    kv[0, tokens:, :] = strip.astype(BF16)

    pl.semaphore_wait(barrier, n + groups - 1)
    shared = {}
    for d in range(n - 1, 0, -1):
        shared[d] = remote(kv.at[0], kv.at[d], {"sp": partners(me, d, n)[0]})
    away = {}
    for j in range(1, groups):
        away[j] = remote(
            down_any, dw_ref.at[pl.ds(2 * j * hidden, hidden)], {"tp": lax.rem(rank + m - 2 * j, m)}
        )
    aside = [
        remote(gate_any, gu_ref.at[:, pl.ds(hidden, hidden)], {"tp": sibling}),
        remote(up_any, gu_ref.at[:, pl.ds(local + hidden, hidden)], {"tp": sibling}),
        remote(down_any, dw_ref.at[pl.ds(hidden, hidden)], {"tp": sibling}),
    ]

    factor = (NOPE + ROPE) ** (-0.5) * LOG2E
    loads["qr"].wait()
    rep_row = lax.broadcasted_iota(jnp.int32, (LANES, LANES * LANES // ROPE), 0)
    rep_col = lax.broadcasted_iota(jnp.int32, (LANES, LANES * LANES // ROPE), 1)
    spread = (
        rep_row == rep_col // LANES * ROPE + rep_col % ROPE
    ).astype(F32).astype(BF16)
    for g in range(HEADS * ROPE // LANES):
        x = qr_ref[:, g * LANES : (g + 1) * LANES].astype(F32)
        x = ((x * cosine + swapped(x) * sine) * factor).astype(BF16)
        x = jnp.dot(x, spread, preferred_element_type=F32).astype(BF16)
        for k in range(LANES // ROPE):
            head = g * (LANES // ROPE) + k
            query[head * tokens : (head + 1) * tokens, LATENT:] = x[:, k * LANES : (k + 1) * LANES]
    lane = lax.broadcasted_iota(jnp.int32, (tokens, LANES), 1)
    below = lane < NOPE
    lowb = below.astype(F32).astype(BF16)
    highb = (lane >= NOPE).astype(F32).astype(BF16)
    loads["qn"].wait()
    loads["upk"].wait()
    for g in range(HEADS * NOPE // LANES):
        plain = qn_ref[:, g * LANES : (g + 1) * LANES]
        pair = jnp.concatenate([plain * lowb, plain * highb], axis=0)
        absorbed = lax.dot_general(
            pair, upk_ref[:, g * LANES : (g + 1) * LANES], BYCOL, preferred_element_type=F32
        )
        query[2 * g * tokens : 2 * (g + 1) * tokens, :LATENT] = (absorbed * factor).astype(BF16)

    loads["picks"].wait()
    loads["share"].wait()
    spots = place(picks_ref, n, slots, tokens)
    packer[...] = sum(spots).astype(BF16)
    coarse = fine = 0.0
    for k in range(TOPK):
        share = share_ref[k : k + 1, :]
        rounded = share.astype(BF16).astype(F32)
        coarse = coarse + spots[k] * rounded
        fine = fine + spots[k] * (share - rounded)
    if pad:
        filler = jnp.zeros((n * slots, pad), F32)
        coarse = jnp.concatenate([coarse, filler], axis=1)
        fine = jnp.concatenate([fine, filler], axis=1)
    high[...] = jnp.transpose(coarse)[:tokens].astype(BF16)
    low[...] = jnp.transpose(fine)[:tokens].astype(BF16)

    vals[:, LATENT:] = jnp.ones((n * tokens, LANES), BF16)
    for d in [0] + list(range(1, n)):
        if d:
            shared[d].wait()
        rows = slice(d * tokens, (d + 1) * tokens)
        keys[rows, :LATENT] = kv[d, :tokens, :]
        vals[rows, :LATENT] = kv[d, :tokens, :]
        strip = kv[d, tokens:, :].astype(F32)[:packed]
        keys[rows, LATENT:] = jnp.concatenate([strip * mask for mask in masks], axis=0).astype(BF16)
    loads["upv"].wait()

    def heads(g, carry):
        lanes = pl.ds(pl.multiple_of(g * LANES, LANES), LANES)
        mine = query[pl.ds(pl.multiple_of(g * 2 * tokens, 2 * tokens), 2 * tokens), :]
        scores = lax.dot_general(mine, keys[...], BYCOL, preferred_element_type=F32)
        weights = jnp.exp2(scores - jnp.max(scores, axis=-1, keepdims=True)).astype(BF16)
        mixed = jnp.dot(weights, vals[...], preferred_element_type=F32)
        mixed = (mixed[:, :LATENT] / mixed[:, LATENT:]).astype(BF16)
        mixed = jnp.dot(mixed, upv_ref[:, lanes], preferred_element_type=F32)
        att[:, lanes] = jnp.where(below, mixed[:tokens], mixed[tokens:]).astype(BF16)
        return carry

    lax.fori_loop(0, HEADS * VDIM // LANES, heads, 0)
    loads["ow"].wait()
    loads["res"].wait()
    loads["fgain"].wait()

    def project(c, square):
        cols = pl.ds(pl.multiple_of(c * step, step), step)
        product = jnp.dot(att[...], ow_ref[:, cols], preferred_element_type=F32)
        middle = (mid_ref[:, cols].astype(F32) + product).astype(BF16)
        mid_ref[:, cols] = middle
        full = middle.astype(F32)
        return square + jnp.sum(full * full, axis=-1, keepdims=True)

    square = lax.fori_loop(0, width // step, project, jnp.zeros((tokens, 1), F32))
    scale = lax.rsqrt(square / width + EPS)
    norm[...] = (mid_ref[...].astype(F32) * scale * fgain_ref[...]).astype(BF16)

    def pack(c, carry):
        cols = pl.ds(pl.multiple_of(c * step, step), step)
        sent[:, cols] = jnp.dot(packer[...], norm[:, cols], preferred_element_type=F32).astype(BF16)
        return carry

    lax.fori_loop(0, width // step, pack, 0)

    def block(index):
        return pl.ds(pl.multiple_of(index * slots, slots), slots)

    arrive, across, crossed, returned = {}, {}, {}, {}
    for p, d in enumerate(order):
        if d:
            peer = partners(me, d, n)[0]
            arrive[d] = remote(sent.at[block(peer)], rows_a.at[block(p)], {"sp": peer})
    rows_a[(n - 1) * slots :, :] = sent[block(me), :]

    def forward(k):
        for p in range(k * count, (k + 1) * count):
            if order[p]:
                arrive[order[p]].wait()
            for j in range(1, groups):
                across[p, j] = remote(
                    rows_a.at[block(p)], rows_b.at[j - 1, block(p)], {"tp": lax.rem(rank + 2 * j, m)}
                )

    def gates(k):
        rows = pl.ds(k * span, span)
        for j in range(1, groups):
            for p in range(k * count, (k + 1) * count):
                across[p, j].wait()
        if k == 0:
            for name in ("gate", "up", "down"):
                loads[name].wait()
            for copy in aside:
                copy.wait()
            for j in range(1, groups):
                away[j].wait()
                away[-j] = remote(
                    dw_ref.at[pl.ds(2 * j * hidden, hidden)],
                    dw_ref.at[pl.ds((2 * j + 1) * hidden, hidden)],
                    {"tp": sibling},
                )
        stack = jnp.concatenate(
            [rows_a[rows, :]] + [rows_b[j - 1, rows, :] for j in range(1, groups)], axis=0
        )
        both = jnp.dot(stack, gu_ref[...], preferred_element_type=F32)
        gate = jnp.minimum(both[:, :local], CLAMP)
        lift = jnp.clip(both[:, local:], -CLAMP, CLAMP)
        active = (gate * jax.nn.sigmoid(ALPHA * gate) * (lift + 1.0)).astype(BF16)
        for j in range(1, groups):
            act_b[j - 1, rows, :] = active[j * span : (j + 1) * span]
            crossed[k, j] = remote(
                act_b.at[j - 1, rows],
                act.at[rows, pl.ds(j * local, local)],
                {"tp": lax.rem(rank + m - 2 * j, m)},
            )
        act[rows, :local] = active[:span]

    def lower(k):
        rows = pl.ds(k * span, span)
        for j in range(1, groups):
            crossed[k, j].wait()
            if k == 0:
                away[-j].wait()

        def down(c, carry):
            cols = pl.ds(pl.multiple_of(c * step, step), step)
            res[rows, cols] = jnp.dot(
                act[rows, :], dw_ref[:, cols], preferred_element_type=F32
            ).astype(BF16)
            return carry

        lax.fori_loop(0, width // step, down, 0)
        for p in range(k * count, (k + 1) * count):
            d = order[p]
            if d:
                returned[d] = remote(
                    res.at[block(p)], back.at[block(me)], {"sp": partners(me, d, n)[1]}
                )
            else:
                back[block(me), :] = res[p * slots : (p + 1) * slots, :]

    for t in range(parts + 2):
        for work, k in ((forward, t), (gates, t - 1), (lower, t - 2)):
            if 0 <= k < parts:
                work(k)
    for d in order:
        if d:
            returned[d].wait()

    def combine(c, carry):
        cols = pl.ds(pl.multiple_of(c * step, step), step)
        rows = back[:, cols]
        added = jnp.dot(high[...], rows, preferred_element_type=F32)
        added = added + jnp.dot(low[...], rows, preferred_element_type=F32)
        out_ref[:, cols] = (mid_ref[:, cols].astype(F32) + added).astype(BF16)
        return carry

    lax.fori_loop(0, width // step, combine, 0)


def rotary_tables(tokens, n):
    half = ROPE // 2
    lane = np.arange(LANES)
    inverse = ROPE_BASE ** (-(lane % half) * 2.0 / ROPE)
    places = np.concatenate([np.arange(tokens), np.arange(n) * tokens]).astype(np.float64)
    angle = places[:, None] * inverse[None, :]
    sign = np.where(lane % ROPE < half, -1.0, 1.0)[None, :]
    return np.stack([np.cos(angle), np.sin(angle) * sign]).astype(np.float32)


def local(
    residual, query_nope, query_rope, latent, rope_key, latent_gain, up_key, up_value,
    out_weight, ffn_gain, routes, route_weight, gate_weight, up_weight, down_weight,
):
    tokens, width = residual.shape[1:]
    hidden = gate_weight.shape[2]
    n = lax.axis_size("sp")
    m = lax.axis_size("tp")
    groups = m // 2
    parts = min(4, n)
    slots = min(tokens, max(2, 5 * tokens * TOPK // (4 * n)))
    slots = -(-slots // 16) * 16
    depth = tokens + tokens // (LANES // ROPE)
    depth = -(-depth // 16) * 16
    tables = jnp.asarray(rotary_tables(tokens, n))
    copies = 3 * (n - 1) + 3 + (groups - 1) * (2 + n + parts)

    def vmem(*shape, dtype=BF16):
        return pltpu.VMEM(shape, dtype)

    updated = pl.pallas_call(
        functools.partial(layer_kernel, n, m, slots, parts),
        out_shape=jax.ShapeDtypeStruct((tokens, width), BF16),
        in_specs=[ANY] * 16,
        out_specs=VM,
        scratch_shapes=[
            vmem(tokens, LATENT),
            vmem(ROPE, tokens),
            vmem(1, LATENT, dtype=F32),
            vmem(*tables.shape, dtype=F32),
            vmem(tokens, HEADS * NOPE),
            vmem(tokens, HEADS * ROPE),
            vmem(LATENT, HEADS * NOPE),
            vmem(LATENT, HEADS * VDIM),
            vmem(HEADS * VDIM, width),
            vmem(tokens, width),
            vmem(1, width, dtype=F32),
            vmem(TOPK, tokens, dtype=jnp.int32),
            vmem(TOPK, tokens, dtype=F32),
            vmem(width, 4 * hidden),
            vmem(m * hidden, width),
            vmem(n, depth, LANES),
            vmem(n * tokens, 2 * LANES),
            vmem(n * tokens, 2 * LANES),
            vmem(HEADS * tokens, 2 * LANES),
            vmem(tokens, HEADS * VDIM),
            vmem(tokens, width),
            vmem(n * slots, tokens),
            vmem(tokens, n * slots),
            vmem(tokens, n * slots),
            vmem(n * slots, width),
            vmem(n * slots, width),
            vmem(max(1, groups - 1), n * slots, width),
            vmem(n * slots, m * hidden),
            vmem(max(1, groups - 1), n * slots, 2 * hidden),
            vmem(n * slots, width),
            vmem(n * slots, width),
            pltpu.SemaphoreType.DMA((16,)),
            pltpu.SemaphoreType.DMA((copies,)),
            pltpu.SemaphoreType.DMA((copies,)),
        ],
        compiler_params=pltpu.CompilerParams(
            collective_id=0, has_side_effects=True, vmem_limit_bytes=60 * 2**20
        ),
    )(
        latent[0], jnp.transpose(rope_key[0]), latent_gain[None, :], tables, query_nope[0],
        query_rope[0], up_key, up_value, out_weight, residual[0], ffn_gain[None, :],
        jnp.transpose(routes, (0, 2, 1)), jnp.transpose(route_weight[0]),
        gate_weight[0], up_weight[0], down_weight[0],
    )
    return updated[None]


def solution(mesh):
    in_specs = (
        P("tp", "sp", None),
        P("tp", "sp", None),
        P("tp", "sp", None),
        P("tp", "sp", None),
        P("tp", "sp", None),
        P(),
        P(),
        P(),
        P(),
        P(),
        P(None, "sp", None),
        P("tp", "sp", None),
        P("sp", None, "tp"),
        P("sp", None, "tp"),
        P("sp", "tp", None),
    )
    out_specs = P("tp", "sp", None)
    return jax.shard_map(local, mesh=mesh, in_specs=in_specs, out_specs=out_specs, check_vma=False)
```

```python
import functools

import jax
import jax.numpy as jnp
import numpy as np
from jax import lax
from jax.experimental import pallas as pl
from jax.experimental.pallas import tpu as pltpu
from jax.sharding import PartitionSpec as P

HEADS = 16
NOPE = 64
ROPE = 32
VDIM = 64
LATENT = 128
TOPK = 2
LANES = 128

EPS = 1e-06
ROPE_BASE = 10000.0
CLAMP = 7.0
ALPHA = 1.702
LOG2E = 1.4426950408889634
MESH = pl.DeviceIdType.MESH
VM = pl.BlockSpec(memory_space=pltpu.VMEM)
ANY = pl.BlockSpec(memory_space=pl.ANY)
F32 = jnp.float32
BF16 = jnp.bfloat16
BYCOL = (((1,), (1,)), ((), ()))


def swapped(x):
    lane = lax.broadcasted_iota(jnp.int32, x.shape, 1)
    half = ROPE // 2
    return jnp.where(
        lane % ROPE < half, pltpu.roll(x, x.shape[1] - half, 1), pltpu.roll(x, half, 1)
    )


def place(picks_ref, experts, slots, tokens):
    expert = lax.broadcasted_iota(jnp.int32, (experts, tokens), 0)
    hots = [(expert == picks_ref[k : k + 1, :]).astype(F32) for k in range(TOPK)]
    earlier = (
        lax.broadcasted_iota(jnp.int32, (tokens, tokens), 0)
        < lax.broadcasted_iota(jnp.int32, (tokens, tokens), 1)
    ).astype(F32)
    rank = jnp.dot(sum(hots), earlier, preferred_element_type=F32)
    where = rank + (expert * slots).astype(F32)
    slot = lax.broadcasted_iota(jnp.int32, (experts * slots, tokens), 0).astype(F32)
    return [
        (slot == jnp.sum(hot * where, axis=0, keepdims=True)).astype(F32) for hot in hots
    ]


def partners(me, d, n):
    if n & (n - 1):
        return lax.rem(me + d, n), lax.rem(me + n - d, n)
    peer, bit = me, 1
    while bit < n:
        if d & bit:
            peer = peer + bit * (1 - 2 * lax.rem(lax.div(me, bit), 2))
        bit *= 2
    return peer, peer


def schedule(n):
    quarter = n // 4
    if n & (n - 1) or not quarter:
        return list(range(n - 1, 0, -1)), list(range(n - 1, -1, -1))
    own, near, mid, far = (list(range((q + 1) * quarter - 1, q * quarter - 1, -1)) for q in range(4))
    return own[:-1] + far + near + mid, far + near + mid + own


def layer_kernel(
    n, m, slots, parts,
    lat_any, rope_any, lgain_any, tab_any, qn_any, qr_any, upk_any, upv_any, ow_any, res_any,
    fgain_any, routes_any, share_any, gate_any, up_any, down_any,
    mid_out, back, high_out, low_out,
    lat_ref, rope_ref, lgain_ref, tab_ref, qn_ref, qr_ref, upk_ref, upv_ref, ow_ref, mid_ref,
    fgain_ref, picks_ref, share_ref, gu_ref, dw_ref,
    kv, keys, vals, query, partial, peaks, att, norm, packer, high, low, sent, rows_a, rows_b, act, act_b, res,
    load_sem, save_sem, send_sem, recv_sem,
):
    tokens, width = mid_out.shape
    hidden = gate_any.shape[1]
    groups = m // 2
    local = 2 * hidden
    me = lax.axis_index("sp")
    rank = lax.axis_index("tp")
    sibling = rank + 1 - 2 * lax.rem(rank, 2)
    count = n // parts
    span = count * slots
    step = 512
    sending, order = schedule(n)
    packed = tokens // (LANES // ROPE)

    barrier = pltpu.get_barrier_semaphore()
    for d in range(1, n):
        pl.semaphore_signal(
            barrier, inc=1, device_id={"sp": partners(me, d, n)[0]}, device_id_type=MESH
        )
    for j in range(1, groups):
        pl.semaphore_signal(
            barrier, inc=1, device_id={"tp": lax.rem(rank + 2 * j, m)}, device_id_type=MESH
        )
    pl.semaphore_signal(barrier, inc=1, device_id={"tp": sibling}, device_id_type=MESH)

    loads = {}

    def load(name, source, target):
        loads[name] = pltpu.make_async_copy(source, target, load_sem.at[len(loads)])
        loads[name].start()

    load("lat", lat_any, lat_ref)
    load("rope", rope_any, rope_ref)
    load("lgain", lgain_any, lgain_ref)
    load("tab", tab_any, tab_ref)
    load("qr", qr_any, qr_ref)
    load("qn", qn_any, qn_ref)
    load("upk", upk_any, upk_ref)
    load("picks", routes_any.at[rank], picks_ref)
    load("share", share_any, share_ref)
    load("upv", upv_any, upv_ref)
    load("ow", ow_any, ow_ref)
    load("res", res_any, mid_ref)
    load("fgain", fgain_any, fgain_ref)
    load("gate", gate_any, gu_ref.at[:, pl.ds(0, hidden)])
    load("up", up_any, gu_ref.at[:, pl.ds(local, hidden)])
    load("down", down_any, dw_ref.at[pl.ds(0, hidden)])

    saves = []

    def save(source, target):
        saves.append(pltpu.make_async_copy(source, target, save_sem.at[len(saves)]))
        saves[-1].start()

    used = [0]

    def remote(source, target, device):
        index = used[0]
        used[0] += 1
        copy = pltpu.make_async_remote_copy(
            src_ref=source,
            dst_ref=target,
            send_sem=send_sem.at[index],
            recv_sem=recv_sem.at[index],
            device_id=device,
            device_id_type=MESH,
        )
        copy.start()
        return copy

    pl.semaphore_wait(barrier, n + groups - 1)
    away = {}
    for j in range(1, groups):
        away[j] = remote(
            down_any, dw_ref.at[pl.ds(2 * j * hidden, hidden)], {"tp": lax.rem(rank + m - 2 * j, m)}
        )

    for name in ("lat", "rope", "lgain", "tab"):
        loads[name].wait()
    base_cos = tab_ref[0, pl.ds(tokens + me, 1), :]
    base_sin = tab_ref[1, pl.ds(tokens + me, 1), :]
    cosine = tab_ref[0, :tokens, :] * base_cos - tab_ref[1, :tokens, :] * base_sin
    sine = tab_ref[1, :tokens, :] * base_cos + tab_ref[0, :tokens, :] * base_sin
    lat = lat_ref[...].astype(F32)
    mean = jnp.mean(lat * lat, axis=-1, keepdims=True)
    kv[0, :tokens, :] = (lat * lax.rsqrt(mean + EPS) * lgain_ref[...]).astype(BF16)
    wide = jnp.concatenate([rope_ref[...].astype(F32)] * (LANES // ROPE), axis=0)
    pad = -tokens % LANES
    if pad:
        wide = jnp.concatenate([wide, jnp.zeros((LANES, pad), F32)], axis=1)
    wide = jnp.transpose(wide)[:tokens]
    turned = wide * cosine + swapped(wide) * sine
    lane = lax.broadcasted_iota(jnp.int32, (packed, LANES), 1)
    masks = [(lane // ROPE == g).astype(F32) for g in range(LANES // ROPE)]
    strip = sum(turned[g * packed : (g + 1) * packed] * masks[g] for g in range(LANES // ROPE))
    rest = kv.shape[1] - tokens - packed
    if rest:
        strip = jnp.concatenate([strip, jnp.zeros((rest, LANES), F32)], axis=0)
    kv[0, tokens:, :] = strip.astype(BF16)

    shared = {}
    for d in range(1, n):
        shared[d] = remote(kv.at[0], kv.at[d], {"sp": partners(me, d, n)[0]})
    aside = [
        remote(gate_any, gu_ref.at[:, pl.ds(hidden, hidden)], {"tp": sibling}),
        remote(up_any, gu_ref.at[:, pl.ds(local + hidden, hidden)], {"tp": sibling}),
        remote(down_any, dw_ref.at[pl.ds(hidden, hidden)], {"tp": sibling}),
    ]

    factor = (NOPE + ROPE) ** (-0.5) * LOG2E
    loads["qr"].wait()
    rep_row = lax.broadcasted_iota(jnp.int32, (LANES, LANES * LANES // ROPE), 0)
    rep_col = lax.broadcasted_iota(jnp.int32, (LANES, LANES * LANES // ROPE), 1)
    spread = (
        rep_row == rep_col // LANES * ROPE + rep_col % ROPE
    ).astype(F32).astype(BF16)
    for g in range(HEADS * ROPE // LANES):
        x = qr_ref[:, g * LANES : (g + 1) * LANES].astype(F32)
        x = ((x * cosine + swapped(x) * sine) * factor).astype(BF16)
        x = jnp.dot(x, spread, preferred_element_type=F32).astype(BF16)
        for k in range(LANES // ROPE):
            head = g * (LANES // ROPE) + k
            query[head * tokens : (head + 1) * tokens, LATENT:] = x[:, k * LANES : (k + 1) * LANES]
    lane = lax.broadcasted_iota(jnp.int32, (tokens, LANES), 1)
    below = lane < NOPE
    lowb = below.astype(F32).astype(BF16)
    highb = (lane >= NOPE).astype(F32).astype(BF16)
    loads["qn"].wait()
    loads["upk"].wait()
    for g in range(HEADS * NOPE // LANES):
        plain = qn_ref[:, g * LANES : (g + 1) * LANES]
        pair = jnp.concatenate([plain * lowb, plain * highb], axis=0)
        absorbed = lax.dot_general(
            pair, upk_ref[:, g * LANES : (g + 1) * LANES], BYCOL, preferred_element_type=F32
        )
        query[2 * g * tokens : 2 * (g + 1) * tokens, :LATENT] = (absorbed * factor).astype(BF16)

    loads["picks"].wait()
    loads["share"].wait()
    spots = place(picks_ref, n, slots, tokens)
    packer[...] = sum(spots).astype(BF16)
    coarse = fine = 0.0
    for k in range(TOPK):
        share = share_ref[k : k + 1, :]
        rounded = share.astype(BF16).astype(F32)
        coarse = coarse + spots[k] * rounded
        fine = fine + spots[k] * (share - rounded)
    if pad:
        filler = jnp.zeros((n * slots, pad), F32)
        coarse = jnp.concatenate([coarse, filler], axis=1)
        fine = jnp.concatenate([fine, filler], axis=1)
    high[...] = jnp.transpose(coarse)[:tokens].astype(BF16)
    low[...] = jnp.transpose(fine)[:tokens].astype(BF16)
    save(high, high_out)
    save(low, low_out)

    vals[:, LATENT:] = jnp.ones((n * tokens, LANES), BF16)

    def unpack(d):
        if d:
            shared[d].wait()
        rows = slice(d * tokens, (d + 1) * tokens)
        keys[rows, :LATENT] = kv[d, :tokens, :]
        vals[rows, :LATENT] = kv[d, :tokens, :]
        strip = kv[d, tokens:, :].astype(F32)[:packed]
        keys[rows, LATENT:] = jnp.concatenate([strip * mask for mask in masks], axis=0).astype(BF16)
    early = max(1, n // 2) * tokens
    total = n * tokens

    def scored(g, start, size):
        mine = query[pl.ds(pl.multiple_of(g * 2 * tokens, 2 * tokens), 2 * tokens), :]
        return lax.dot_general(
            mine, keys[start : start + size, :], BYCOL, preferred_element_type=F32
        )

    def first(g, carry):
        rows = pl.ds(pl.multiple_of(g * 2 * tokens, 2 * tokens), 2 * tokens)
        scores = scored(g, 0, early)
        peak = jnp.max(scores, axis=-1, keepdims=True)
        weights = jnp.exp2(scores - peak).astype(BF16)
        partial[rows, :] = jnp.dot(weights, vals[:early, :], preferred_element_type=F32)
        peaks[rows, :] = jnp.broadcast_to(peak, (2 * tokens, LANES))
        return carry

    def second(g, carry):
        lanes = pl.ds(pl.multiple_of(g * LANES, LANES), LANES)
        rows = pl.ds(pl.multiple_of(g * 2 * tokens, 2 * tokens), 2 * tokens)
        scores = scored(g, early, total - early)
        before = peaks[rows, :]
        peak = jnp.maximum(before[:, :1], jnp.max(scores, axis=-1, keepdims=True))
        weights = jnp.exp2(scores - peak).astype(BF16)
        keep = jnp.exp2(before - peak)
        mixed = jnp.dot(weights, vals[early:, :], preferred_element_type=F32)
        above = mixed[:, :LATENT] + keep * partial[rows, :LATENT]
        under = mixed[:, LATENT:] + keep * partial[rows, LATENT:]
        mixed = (above / under).astype(BF16)
        mixed = jnp.dot(mixed, upv_ref[:, lanes], preferred_element_type=F32)
        att[:, lanes] = jnp.where(below, mixed[:tokens], mixed[tokens:]).astype(BF16)
        return carry

    pairs = HEADS * VDIM // LANES
    for d in range(early // tokens):
        unpack(d)
    lax.fori_loop(0, pairs, first, 0, unroll=4)
    for d in range(early // tokens, n):
        unpack(d)
    loads["upv"].wait()
    lax.fori_loop(0, pairs, second, 0, unroll=4)
    loads["ow"].wait()
    loads["res"].wait()
    loads["fgain"].wait()

    def project(c, square):
        cols = pl.ds(pl.multiple_of(c * step, step), step)
        product = jnp.dot(att[...], ow_ref[:, cols], preferred_element_type=F32)
        middle = (mid_ref[:, cols].astype(F32) + product).astype(BF16)
        mid_ref[:, cols] = middle
        full = middle.astype(F32)
        return square + jnp.sum(full * full, axis=-1, keepdims=True)

    square = lax.fori_loop(0, width // step, project, jnp.zeros((tokens, 1), F32), unroll=2)
    scale = lax.rsqrt(square / width + EPS)
    norm[...] = (mid_ref[...].astype(F32) * scale * fgain_ref[...]).astype(BF16)

    save(mid_ref, mid_out)

    def pack(c, carry):
        cols = pl.ds(pl.multiple_of(c * step, step), step)
        sent[:, cols] = jnp.dot(packer[...], norm[:, cols], preferred_element_type=F32).astype(BF16)
        return carry

    lax.fori_loop(0, width // step, pack, 0, unroll=2)

    def block(index):
        return pl.ds(pl.multiple_of(index * slots, slots), slots)

    arrive, across, crossed, returned = {}, {}, {}, {}
    for d in sending:
        peer = partners(me, d, n)[0]
        arrive[d] = remote(sent.at[block(peer)], rows_a.at[block(order.index(d))], {"sp": peer})
    rows_a[block(order.index(0)), :] = sent[block(me), :]

    def forward(k):
        for p in range(k * count, (k + 1) * count):
            if order[p]:
                arrive[order[p]].wait()
            for j in range(1, groups):
                across[p, j] = remote(
                    rows_a.at[block(p)], rows_b.at[j - 1, block(p)], {"tp": lax.rem(rank + 2 * j, m)}
                )

    def gates(k):
        rows = pl.ds(k * span, span)
        for j in range(1, groups):
            for p in range(k * count, (k + 1) * count):
                across[p, j].wait()
        if k == 0:
            for name in ("gate", "up", "down"):
                loads[name].wait()
            for copy in aside:
                copy.wait()
            for j in range(1, groups):
                away[j].wait()
                away[-j] = remote(
                    dw_ref.at[pl.ds(2 * j * hidden, hidden)],
                    dw_ref.at[pl.ds((2 * j + 1) * hidden, hidden)],
                    {"tp": sibling},
                )
        stack = jnp.concatenate(
            [rows_a[rows, :]] + [rows_b[j - 1, rows, :] for j in range(1, groups)], axis=0
        )
        both = jnp.dot(stack, gu_ref[...], preferred_element_type=F32)
        gate = jnp.minimum(both[:, :local], CLAMP)
        lift = jnp.clip(both[:, local:], -CLAMP, CLAMP)
        active = (gate * jax.nn.sigmoid(ALPHA * gate) * (lift + 1.0)).astype(BF16)
        for j in range(1, groups):
            act_b[j - 1, rows, :] = active[j * span : (j + 1) * span]
            crossed[k, j] = remote(
                act_b.at[j - 1, rows],
                act.at[rows, pl.ds(j * local, local)],
                {"tp": lax.rem(rank + m - 2 * j, m)},
            )
        act[rows, :local] = active[:span]

    def lower(k):
        rows = pl.ds(k * span, span)
        for j in range(1, groups):
            crossed[k, j].wait()
            if k == 0:
                away[-j].wait()

        def down(c, carry):
            cols = pl.ds(pl.multiple_of(c * step, step), step)
            res[rows, cols] = jnp.dot(
                act[rows, :], dw_ref[:, cols], preferred_element_type=F32
            ).astype(BF16)
            return carry

        lax.fori_loop(0, width // step, down, 0, unroll=True)
        for p in range(k * count, (k + 1) * count):
            d = order[p]
            if d:
                returned[d] = remote(
                    res.at[block(p)], back.at[block(me)], {"sp": partners(me, d, n)[1]}
                )
            else:
                save(res.at[block(p)], back.at[block(me)])

    for t in range(parts + 2):
        for work, k in ((forward, t), (gates, t - 1), (lower, t - 2)):
            if 0 <= k < parts:
                work(k)
    for d in order:
        if d:
            returned[d].wait()

    for copy in saves:
        copy.wait()


def combine_kernel(
    back_any, mid_any, high_any, low_any, out_any, back_ref, mid_ref, high_ref, low_ref, out_ref,
    load_sem, save_sem,
):
    width = out_ref.shape[1]
    chunks = save_sem.shape[0]
    step = width // chunks
    pieces = [pl.ds(c * step, step) for c in range(chunks)]
    copies = [
        pltpu.make_async_copy(high_any, high_ref, load_sem.at[0]),
        pltpu.make_async_copy(low_any, low_ref, load_sem.at[1]),
    ]
    for c, cols in enumerate(pieces):
        copies.append(
            pltpu.make_async_copy(back_any.at[:, cols], back_ref.at[:, cols], load_sem.at[2 + 2 * c])
        )
        copies.append(
            pltpu.make_async_copy(mid_any.at[:, cols], mid_ref.at[:, cols], load_sem.at[3 + 2 * c])
        )
    for copy in copies:
        copy.start()
    copies[0].wait()
    copies[1].wait()
    saves = []
    for c, cols in enumerate(pieces):
        copies[2 + 2 * c].wait()
        copies[3 + 2 * c].wait()
        rows = back_ref[:, cols]
        added = jnp.dot(high_ref[...], rows, preferred_element_type=F32)
        added = added + jnp.dot(low_ref[...], rows, preferred_element_type=F32)
        out_ref[:, cols] = (mid_ref[:, cols].astype(F32) + added).astype(BF16)
        saves.append(
            pltpu.make_async_copy(out_ref.at[:, cols], out_any.at[:, cols], save_sem.at[c])
        )
        saves[-1].start()
    for copy in saves:
        copy.wait()


def rotary_tables(tokens, n):
    half = ROPE // 2
    lane = np.arange(LANES)
    inverse = ROPE_BASE ** (-(lane % half) * 2.0 / ROPE)
    places = np.concatenate([np.arange(tokens), np.arange(n) * tokens]).astype(np.float64)
    angle = places[:, None] * inverse[None, :]
    sign = np.where(lane % ROPE < half, -1.0, 1.0)[None, :]
    return np.stack([np.cos(angle), np.sin(angle) * sign]).astype(np.float32)


def local(
    residual, query_nope, query_rope, latent, rope_key, latent_gain, up_key, up_value,
    out_weight, ffn_gain, routes, route_weight, gate_weight, up_weight, down_weight,
):
    tokens, width = residual.shape[1:]
    hidden = gate_weight.shape[2]
    n = lax.axis_size("sp")
    m = lax.axis_size("tp")
    groups = m // 2
    parts = min(8, n)
    slots = min(tokens, max(2, 5 * tokens * TOPK // (4 * n)))
    slots = -(-slots // 16) * 16
    depth = tokens + tokens // (LANES // ROPE)
    depth = -(-depth // 16) * 16
    tables = jnp.asarray(rotary_tables(tokens, n))
    copies = 3 * (n - 1) + 3 + (groups - 1) * (2 + n + parts)

    def vmem(*shape, dtype=BF16):
        return pltpu.VMEM(shape, dtype)

    middle, back, high, low = pl.pallas_call(
        functools.partial(layer_kernel, n, m, slots, parts),
        out_shape=(
            jax.ShapeDtypeStruct((tokens, width), BF16),
            jax.ShapeDtypeStruct((n * slots, width), BF16),
            jax.ShapeDtypeStruct((tokens, n * slots), BF16),
            jax.ShapeDtypeStruct((tokens, n * slots), BF16),
        ),
        in_specs=[ANY] * 16,
        out_specs=(ANY,) * 4,
        scratch_shapes=[
            vmem(tokens, LATENT),
            vmem(ROPE, tokens),
            vmem(1, LATENT, dtype=F32),
            vmem(*tables.shape, dtype=F32),
            vmem(tokens, HEADS * NOPE),
            vmem(tokens, HEADS * ROPE),
            vmem(LATENT, HEADS * NOPE),
            vmem(LATENT, HEADS * VDIM),
            vmem(HEADS * VDIM, width),
            vmem(tokens, width),
            vmem(1, width, dtype=F32),
            vmem(TOPK, tokens, dtype=jnp.int32),
            vmem(TOPK, tokens, dtype=F32),
            vmem(width, 4 * hidden),
            vmem(m * hidden, width),
            vmem(n, depth, LANES),
            vmem(n * tokens, 2 * LANES),
            vmem(n * tokens, 2 * LANES),
            vmem(HEADS * tokens, 2 * LANES),
            vmem(HEADS * tokens, 2 * LANES, dtype=F32),
            vmem(HEADS * tokens, LANES, dtype=F32),
            vmem(tokens, HEADS * VDIM),
            vmem(tokens, width),
            vmem(n * slots, tokens),
            vmem(tokens, n * slots),
            vmem(tokens, n * slots),
            vmem(n * slots, width),
            vmem(n * slots, width),
            vmem(max(1, groups - 1), n * slots, width),
            vmem(n * slots, m * hidden),
            vmem(max(1, groups - 1), n * slots, 2 * hidden),
            vmem(n * slots, width),
            pltpu.SemaphoreType.DMA((16,)),
            pltpu.SemaphoreType.DMA((4,)),
            pltpu.SemaphoreType.DMA((copies,)),
            pltpu.SemaphoreType.DMA((copies,)),
        ],
        compiler_params=pltpu.CompilerParams(
            collective_id=0, has_side_effects=True, vmem_limit_bytes=60 * 2**20
        ),
    )(
        latent[0], jnp.transpose(rope_key[0]), latent_gain[None, :], tables, query_nope[0],
        query_rope[0], up_key, up_value, out_weight, residual[0], ffn_gain[None, :],
        jnp.transpose(routes, (0, 2, 1)), jnp.transpose(route_weight[0]),
        gate_weight[0], up_weight[0], down_weight[0],
    )
    chunks = max(1, width // 512)
    updated = pl.pallas_call(
        combine_kernel,
        out_shape=jax.ShapeDtypeStruct((tokens, width), BF16),
        in_specs=[ANY] * 4,
        out_specs=ANY,
        scratch_shapes=[
            vmem(n * slots, width),
            vmem(tokens, width),
            vmem(tokens, n * slots),
            vmem(tokens, n * slots),
            vmem(tokens, width),
            pltpu.SemaphoreType.DMA((2 + 2 * chunks,)),
            pltpu.SemaphoreType.DMA((chunks,)),
        ],
        compiler_params=pltpu.CompilerParams(vmem_limit_bytes=60 * 2**20),
    )(back, middle, high, low)
    return updated[None]


def solution(mesh):
    in_specs = (
        P("tp", "sp", None),
        P("tp", "sp", None),
        P("tp", "sp", None),
        P("tp", "sp", None),
        P("tp", "sp", None),
        P(),
        P(),
        P(),
        P(),
        P(),
        P(None, "sp", None),
        P("tp", "sp", None),
        P("sp", None, "tp"),
        P("sp", None, "tp"),
        P("sp", "tp", None),
    )
    out_specs = P("tp", "sp", None)
    return jax.shard_map(local, mesh=mesh, in_specs=in_specs, out_specs=out_specs, check_vma=False)
```

```python
import functools

import jax
import jax.numpy as jnp
import numpy as np
from jax import lax
from jax.experimental import pallas as pl
from jax.experimental.pallas import tpu as pltpu
from jax.sharding import PartitionSpec as P

HEADS = 16
NOPE = 64
ROPE = 32
VDIM = 64
LATENT = 128
TOPK = 2
LANES = 128

EPS = 1e-06
ROPE_BASE = 10000.0
CLAMP = 7.0
ALPHA = 1.702
LOG2E = 1.4426950408889634
MESH = pl.DeviceIdType.MESH
VM = pl.BlockSpec(memory_space=pltpu.VMEM)
ANY = pl.BlockSpec(memory_space=pl.ANY)
HBM = pl.BlockSpec(memory_space=pltpu.HBM)
F32 = jnp.float32
BF16 = jnp.bfloat16
BYCOL = (((1,), (1,)), ((), ()))


def swapped(x):
    lane = lax.broadcasted_iota(jnp.int32, x.shape, 1)
    half = ROPE // 2
    return jnp.where(
        lane % ROPE < half, pltpu.roll(x, x.shape[1] - half, 1), pltpu.roll(x, half, 1)
    )


def place(picks_ref, experts, slots, tokens):
    expert = lax.broadcasted_iota(jnp.int32, (experts, tokens), 0)
    hots = [(expert == picks_ref[k : k + 1, :]).astype(F32) for k in range(TOPK)]
    earlier = (
        lax.broadcasted_iota(jnp.int32, (tokens, tokens), 0)
        < lax.broadcasted_iota(jnp.int32, (tokens, tokens), 1)
    ).astype(F32)
    rank = jnp.dot(sum(hots), earlier, preferred_element_type=F32)
    where = rank + (expert * slots).astype(F32)
    slot = lax.broadcasted_iota(jnp.int32, (experts * slots, tokens), 0).astype(F32)
    return [
        (slot == jnp.sum(hot * where, axis=0, keepdims=True)).astype(F32) for hot in hots
    ]


def partners(me, d, n):
    if n & (n - 1):
        return lax.rem(me + d, n), lax.rem(me + n - d, n)
    peer, bit = me, 1
    while bit < n:
        if d & bit:
            peer = peer + bit * (1 - 2 * lax.rem(lax.div(me, bit), 2))
        bit *= 2
    return peer, peer


def schedule(n):
    quarter = n // 4
    if n & (n - 1) or not quarter:
        return list(range(n - 1, 0, -1)), list(range(n - 1, -1, -1))
    own, near, mid, far = (list(range((q + 1) * quarter - 1, q * quarter - 1, -1)) for q in range(4))
    mixed = near[:1] + [d for pair in zip(mid, near[1:]) for d in pair] + mid[len(near) - 1 :]
    return own[:-1] + far + near + mid, far + mixed + own


def layer_kernel(
    n, m, slots, parts,
    lat_any, rope_any, lgain_any, tab_any, qn_any, qr_any, upk_any, upv_any, ow_any, res_any,
    fgain_any, routes_any, share_any, gate_any, up_any, down_any,
    mid_ref, back, high, low,
    lat_ref, rope_ref, lgain_ref, tab_ref, qn_ref, qr_ref, upk_ref, upv_ref, ow_ref,
    fgain_ref, picks_ref, share_ref, gu_ref, dw_ref,
    kv, keys, vals, query, partial, peaks, att, norm, packer, sent, rows_a, rows_b, act, act_b, res,
    load_sem, send_sem, recv_sem,
):
    tokens, width = mid_ref.shape
    hidden = gate_any.shape[1]
    groups = m // 2
    local = 2 * hidden
    me = lax.axis_index("sp")
    rank = lax.axis_index("tp")
    sibling = rank + 1 - 2 * lax.rem(rank, 2)
    count = n // parts
    span = count * slots
    step = 512
    sending, order = schedule(n)
    packed = tokens // (LANES // ROPE)

    barrier = pltpu.get_barrier_semaphore()
    for d in range(1, n):
        pl.semaphore_signal(
            barrier, inc=1, device_id={"sp": partners(me, d, n)[0]}, device_id_type=MESH
        )
    for j in range(1, groups):
        pl.semaphore_signal(
            barrier, inc=1, device_id={"tp": lax.rem(rank + 2 * j, m)}, device_id_type=MESH
        )
    pl.semaphore_signal(barrier, inc=1, device_id={"tp": sibling}, device_id_type=MESH)

    loads = [[] for _ in range(5)]

    def load(group, source, target):
        index = sum(len(copies) for copies in loads)
        copy = pltpu.make_async_copy(source, target, load_sem.at[index])
        copy.start()
        loads[group].append(copy)

    def loaded(group):
        for copy in loads[group]:
            copy.wait()

    load(0, lat_any, lat_ref)
    load(0, rope_any, rope_ref)
    load(0, lgain_any, lgain_ref)
    load(0, tab_any, tab_ref)
    load(1, qr_any, qr_ref)
    load(1, qn_any, qn_ref)
    load(1, upk_any, upk_ref)
    load(1, routes_any.at[rank], picks_ref)
    load(1, share_any, share_ref)
    load(2, upv_any, upv_ref)
    load(3, ow_any, ow_ref)
    load(3, res_any, mid_ref)
    load(3, fgain_any, fgain_ref)
    load(4, gate_any, gu_ref.at[:, pl.ds(0, hidden)])
    load(4, up_any, gu_ref.at[:, pl.ds(local, hidden)])
    load(4, down_any, dw_ref.at[pl.ds(0, hidden)])

    used = [0]

    def fresh(count=1):
        used[0] += count
        return used[0] - count

    def remote(source, target, device, leaves, index=None):
        copy = pltpu.make_async_remote_copy(
            src_ref=source,
            dst_ref=target,
            send_sem=send_sem.at[leaves],
            recv_sem=recv_sem.at[fresh() if index is None else index],
            device_id=device,
            device_id_type=MESH,
        )
        copy.start()
        return copy

    def together(extent, index, semaphores):
        pltpu.make_async_copy(extent, extent, semaphores.at[index]).wait()

    kv_out, aside_out, rows_out, back_out = range(4)
    away_out, relay_out, across_out, act_out = (4 + q * (groups - 1) - 1 for q in range(4))

    pl.semaphore_wait(barrier, n + groups - 1)
    away = {}
    for j in range(1, groups):
        away[j] = remote(
            down_any, dw_ref.at[pl.ds(2 * j * hidden, hidden)], {"tp": lax.rem(rank + m - 2 * j, m)},
            away_out + j,
        )

    loaded(0)
    base_cos = tab_ref[0, pl.ds(tokens + me, 1), :]
    base_sin = tab_ref[1, pl.ds(tokens + me, 1), :]
    cosine = tab_ref[0, :tokens, :] * base_cos - tab_ref[1, :tokens, :] * base_sin
    sine = tab_ref[1, :tokens, :] * base_cos + tab_ref[0, :tokens, :] * base_sin
    lat = lat_ref[...].astype(F32)
    mean = jnp.mean(lat * lat, axis=-1, keepdims=True)
    kv[0, :tokens, :] = (lat * lax.rsqrt(mean + EPS) * lgain_ref[...]).astype(BF16)
    wide = jnp.concatenate([rope_ref[...].astype(F32)] * (LANES // ROPE), axis=0)
    pad = -tokens % LANES
    if pad:
        wide = jnp.concatenate([wide, jnp.zeros((LANES, pad), F32)], axis=1)
    wide = jnp.transpose(wide)[:tokens]
    turned = wide * cosine + swapped(wide) * sine
    lane = lax.broadcasted_iota(jnp.int32, (packed, LANES), 1)
    masks = [(lane // ROPE == g).astype(F32) for g in range(LANES // ROPE)]
    strip = sum(turned[g * packed : (g + 1) * packed] * masks[g] for g in range(LANES // ROPE))
    rest = kv.shape[1] - tokens - packed
    if rest:
        strip = jnp.concatenate([strip, jnp.zeros((rest, LANES), F32)], axis=0)
    kv[0, tokens:, :] = strip.astype(BF16)

    shared, soon, late = {}, fresh(), fresh()
    for d in range(1, n):
        half = soon if d < max(1, n // 2) else late
        shared[d] = remote(kv.at[0], kv.at[d], {"sp": partners(me, d, n)[0]}, kv_out, half)
    pack_sem, back_sem = fresh(), fresh()
    aside = [
        remote(gate_any, gu_ref.at[:, pl.ds(hidden, hidden)], {"tp": sibling}, aside_out, pack_sem),
        remote(up_any, gu_ref.at[:, pl.ds(local + hidden, hidden)], {"tp": sibling}, aside_out, pack_sem),
        remote(down_any, dw_ref.at[pl.ds(hidden, hidden)], {"tp": sibling}, aside_out, pack_sem),
    ]

    factor = (NOPE + ROPE) ** (-0.5) * LOG2E
    loaded(1)
    rep_row = lax.broadcasted_iota(jnp.int32, (LANES, LANES * LANES // ROPE), 0)
    rep_col = lax.broadcasted_iota(jnp.int32, (LANES, LANES * LANES // ROPE), 1)
    spread = (
        rep_row == rep_col // LANES * ROPE + rep_col % ROPE
    ).astype(F32).astype(BF16)
    for g in range(HEADS * ROPE // LANES):
        x = qr_ref[:, g * LANES : (g + 1) * LANES].astype(F32)
        x = ((x * cosine + swapped(x) * sine) * factor).astype(BF16)
        x = jnp.dot(x, spread, preferred_element_type=F32).astype(BF16)
        for k in range(LANES // ROPE):
            head = g * (LANES // ROPE) + k
            query[head * tokens : (head + 1) * tokens, LATENT:] = x[:, k * LANES : (k + 1) * LANES]
    lane = lax.broadcasted_iota(jnp.int32, (tokens, LANES), 1)
    below = lane < NOPE
    lowb = below.astype(F32).astype(BF16)
    highb = (lane >= NOPE).astype(F32).astype(BF16)
    for g in range(HEADS * NOPE // LANES):
        plain = qn_ref[:, g * LANES : (g + 1) * LANES]
        pair = jnp.concatenate([plain * lowb, plain * highb], axis=0)
        absorbed = lax.dot_general(
            pair, upk_ref[:, g * LANES : (g + 1) * LANES], BYCOL, preferred_element_type=F32
        )
        query[2 * g * tokens : 2 * (g + 1) * tokens, :LATENT] = (absorbed * factor).astype(BF16)

    spots = place(picks_ref, n, slots, tokens)
    packer[...] = sum(spots).astype(BF16)
    coarse = fine = 0.0
    for k in range(TOPK):
        share = share_ref[k : k + 1, :]
        rounded = share.astype(BF16).astype(F32)
        coarse = coarse + spots[k] * rounded
        fine = fine + spots[k] * (share - rounded)
    if pad:
        filler = jnp.zeros((n * slots, pad), F32)
        coarse = jnp.concatenate([coarse, filler], axis=1)
        fine = jnp.concatenate([fine, filler], axis=1)
    high[...] = jnp.transpose(coarse)[:tokens].astype(BF16)
    low[...] = jnp.transpose(fine)[:tokens].astype(BF16)

    vals[:, LATENT:] = jnp.ones((n * tokens, LANES), BF16)

    def unpack(d):
        rows = slice(d * tokens, (d + 1) * tokens)
        keys[rows, :LATENT] = kv[d, :tokens, :]
        vals[rows, :LATENT] = kv[d, :tokens, :]
        strip = kv[d, tokens:, :].astype(F32)[:packed]
        keys[rows, LATENT:] = jnp.concatenate([strip * mask for mask in masks], axis=0).astype(BF16)
    soonest = max(1, n // 2)
    early = soonest * tokens
    total = n * tokens

    quad = 4 * tokens

    def scored(g, start, size):
        mine = query[pl.ds(pl.multiple_of(g * quad, quad), quad), :]
        return lax.dot_general(
            mine, keys[start : start + size, :], BYCOL, preferred_element_type=F32
        )

    def first(g, carry):
        rows = pl.ds(pl.multiple_of(g * quad, quad), quad)
        scores = scored(g, 0, early)
        peak = jnp.max(scores, axis=-1, keepdims=True)
        weights = jnp.exp2(scores - peak).astype(BF16)
        partial[rows, :] = jnp.dot(weights, vals[:early, :], preferred_element_type=F32)
        peaks[rows, :] = jnp.broadcast_to(peak, (quad, LANES))
        return carry

    def second(g, carry):
        rows = pl.ds(pl.multiple_of(g * quad, quad), quad)
        scores = scored(g, early, total - early)
        before = peaks[rows, :]
        peak = jnp.max(scores, axis=-1, keepdims=True)
        peak = jnp.maximum(before, jnp.broadcast_to(peak, before.shape))
        level = jnp.concatenate([peak] * -(-scores.shape[1] // LANES), axis=1)
        weights = jnp.exp2(scores - level[:, : scores.shape[1]]).astype(BF16)
        keep = jnp.exp2(before - peak)
        mixed = jnp.dot(weights, vals[early:, :], preferred_element_type=F32)
        above = mixed[:, :LATENT] + keep * partial[rows, :LATENT]
        under = mixed[:, LATENT:] + keep * partial[rows, LATENT:]
        mixed = above.astype(BF16)
        for q in range(2):
            lanes = pl.ds(pl.multiple_of((g * 2 + q) * LANES, LANES), LANES)
            part = mixed[2 * q * tokens : 2 * (q + 1) * tokens]
            part = jnp.dot(part, upv_ref[:, lanes], preferred_element_type=F32)
            over = under[2 * q * tokens : 2 * (q + 1) * tokens]
            part = jnp.where(below, part[:tokens], part[tokens:])
            over = jnp.where(below, over[:tokens], over[tokens:])
            att[:, lanes] = (part / over).astype(BF16)
        return carry

    pairs = HEADS // 4
    if soonest > 1:
        together(kv.at[pl.ds(1, soonest - 1)], soon, recv_sem)
    for d in range(soonest):
        unpack(d)
    lax.fori_loop(0, pairs, first, 0, unroll=True)
    together(kv.at[pl.ds(soonest, n - soonest)], late, recv_sem)
    for d in range(soonest, n):
        unpack(d)
    loaded(2)
    lax.fori_loop(0, pairs, second, 0, unroll=2)
    loaded(3)

    def project(c, square):
        cols = pl.ds(pl.multiple_of(c * step, step), step)
        product = jnp.dot(att[...], ow_ref[:, cols], preferred_element_type=F32)
        middle = (mid_ref[:, cols].astype(F32) + product).astype(BF16)
        mid_ref[:, cols] = middle
        full = middle.astype(F32)
        return square + jnp.sum(full * full, axis=-1, keepdims=True)

    square = lax.fori_loop(0, width // step, project, jnp.zeros((tokens, 1), F32), unroll=2)
    scale = lax.rsqrt(square / width + EPS)
    norm[...] = (mid_ref[...].astype(F32) * scale * fgain_ref[...]).astype(BF16)


    def pack(c, carry):
        cols = pl.ds(pl.multiple_of(c * step, step), step)
        sent[:, cols] = jnp.dot(packer[...], norm[:, cols], preferred_element_type=F32).astype(BF16)
        return carry

    lax.fori_loop(0, width // step, pack, 0, unroll=2)

    def block(index):
        return pl.ds(pl.multiple_of(index * slots, slots), slots)

    arrive, across, crossed, returned = {}, {}, {}, {}
    for d in sending:
        peer = partners(me, d, n)[0]
        arrive[d] = remote(sent.at[block(peer)], rows_a.at[block(order.index(d))], {"sp": peer}, rows_out)
    rows_a[block(order.index(0)), :] = sent[block(me), :]

    def forward(k):
        for p in range(k * count, (k + 1) * count):
            if order[p]:
                arrive[order[p]].wait_recv()
            for j in range(1, groups):
                across[p, j] = remote(
                    rows_a.at[block(p)], rows_b.at[j - 1, block(p)], {"tp": lax.rem(rank + 2 * j, m)},
                    across_out + j,
                )

    def gates(k):
        rows = pl.ds(k * span, span)
        for j in range(1, groups):
            for p in range(k * count, (k + 1) * count):
                across[p, j].wait_recv()
        if k == 0:
            loaded(4)
            together(dw_ref.at[pl.ds(0, 3 * hidden)], pack_sem, recv_sem)
            for j in range(1, groups):
                away[j].wait_recv()
                away[-j] = remote(
                    dw_ref.at[pl.ds(2 * j * hidden, hidden)],
                    dw_ref.at[pl.ds((2 * j + 1) * hidden, hidden)],
                    {"tp": sibling},
                    relay_out + j,
                )
        stack = jnp.concatenate(
            [rows_a[rows, :]] + [rows_b[j - 1, rows, :] for j in range(1, groups)], axis=0
        )
        both = jnp.dot(stack, gu_ref[...], preferred_element_type=F32)
        gate = jnp.minimum(both[:, :local], CLAMP)
        lift = jnp.clip(both[:, local:], -CLAMP, CLAMP)
        active = (gate * jax.nn.sigmoid(ALPHA * gate) * (lift + 1.0)).astype(BF16)
        for j in range(1, groups):
            act_b[j - 1, rows, :] = active[j * span : (j + 1) * span]
            crossed[k, j] = remote(
                act_b.at[j - 1, rows],
                act.at[rows, pl.ds(j * local, local)],
                {"tp": lax.rem(rank + m - 2 * j, m)},
                act_out + j,
            )
        act[rows, :local] = active[:span]

    def lower(k):
        rows = pl.ds(k * span, span)
        for j in range(1, groups):
            crossed[k, j].wait_recv()
            if k == 0:
                away[-j].wait_recv()

        def down(c, carry):
            cols = pl.ds(pl.multiple_of(c * step, step), step)
            res[rows, cols] = jnp.dot(
                act[rows, :], dw_ref[:, cols], preferred_element_type=F32
            ).astype(BF16)
            return carry

        lax.fori_loop(0, width // step, down, 0, unroll=True)
        for p in range(k * count, (k + 1) * count):
            d = order[p]
            if d:
                returned[d] = remote(
                    res.at[block(p)], back.at[block(me)], {"sp": partners(me, d, n)[1]}, back_out,
                    back_sem,
                )
            else:
                back[block(me), :] = res[p * slots : (p + 1) * slots, :]

    for t in range(parts + 2):
        for work, k in ((forward, t), (gates, t - 1), (lower, t - 2)):
            if 0 <= k < parts:
                work(k)
    others = pl.ds(0, (n - 1) * slots)
    together(back.at[others], back_sem, recv_sem)
    together(kv.at[pl.ds(0, n - 1)], kv_out, send_sem)
    together(dw_ref.at[pl.ds(0, 3 * hidden)], aside_out, send_sem)
    together(rows_a.at[others], rows_out, send_sem)
    together(back.at[others], back_out, send_sem)
    for j in range(1, groups):
        together(dw_ref.at[pl.ds(0, hidden)], away_out + j, send_sem)
        together(dw_ref.at[pl.ds(0, hidden)], relay_out + j, send_sem)
        together(rows_a, across_out + j, send_sem)
        together(act_b.at[j - 1], act_out + j, send_sem)


def combine_kernel(back_ref, mid_ref, high_ref, low_ref, out_any, out_ref, save_sem):
    width = out_ref.shape[1]
    chunks = save_sem.shape[0]
    step = width // chunks
    saves = []
    for c in range(chunks):
        cols = pl.ds(c * step, step)
        rows = back_ref[:, cols]
        added = jnp.dot(high_ref[...], rows, preferred_element_type=F32)
        added = added + jnp.dot(low_ref[...], rows, preferred_element_type=F32)
        out_ref[:, cols] = (mid_ref[:, cols].astype(F32) + added).astype(BF16)
        saves.append(
            pltpu.make_async_copy(out_ref.at[:, cols], out_any.at[:, cols], save_sem.at[c])
        )
        saves[-1].start()
    for copy in saves:
        copy.wait()


def rotary_tables(tokens, n):
    half = ROPE // 2
    lane = np.arange(LANES)
    inverse = ROPE_BASE ** (-(lane % half) * 2.0 / ROPE)
    places = np.concatenate([np.arange(tokens), np.arange(n) * tokens]).astype(np.float64)
    angle = places[:, None] * inverse[None, :]
    sign = np.where(lane % ROPE < half, -1.0, 1.0)[None, :]
    return np.stack([np.cos(angle), np.sin(angle) * sign]).astype(np.float32)


def local(
    residual, query_nope, query_rope, latent, rope_key, latent_gain, up_key, up_value,
    out_weight, ffn_gain, routes, route_weight, gate_weight, up_weight, down_weight,
):
    tokens, width = residual.shape[1:]
    hidden = gate_weight.shape[2]
    n = lax.axis_size("sp")
    m = lax.axis_size("tp")
    groups = m // 2
    parts = min(8, n)
    slots = min(tokens, max(2, 5 * tokens * TOPK // (4 * n)))
    slots = -(-slots // 16) * 16
    depth = tokens + tokens // (LANES // ROPE)
    depth = -(-depth // 16) * 16
    tables = jnp.asarray(rotary_tables(tokens, n))
    signals = n - 1 + 4 + (groups - 1) * (2 + n + parts)
    leaving = 4 * groups

    room = [16 * 2**20]

    def vmem(*shape, dtype=BF16):
        room[0] += int(np.prod(shape)) * jnp.dtype(dtype).itemsize
        return pltpu.VMEM(shape, dtype)

    scratch = [
        vmem(tokens, LATENT),
        vmem(ROPE, tokens),
        vmem(1, LATENT, dtype=F32),
        vmem(*tables.shape, dtype=F32),
        vmem(tokens, HEADS * NOPE),
        vmem(tokens, HEADS * ROPE),
        vmem(LATENT, HEADS * NOPE),
        vmem(LATENT, HEADS * VDIM),
        vmem(HEADS * VDIM, width),
        vmem(1, width, dtype=F32),
        vmem(TOPK, tokens, dtype=jnp.int32),
        vmem(TOPK, tokens, dtype=F32),
        vmem(width, 4 * hidden),
        vmem(m * hidden, width),
        vmem(n, depth, LANES),
        vmem(n * tokens, 2 * LANES),
        vmem(n * tokens, 2 * LANES),
        vmem(HEADS * tokens, 2 * LANES),
        vmem(HEADS * tokens, 2 * LANES, dtype=F32),
        vmem(HEADS * tokens, LANES, dtype=F32),
        vmem(tokens, HEADS * VDIM),
        vmem(tokens, width),
        vmem(n * slots, tokens),
        vmem(n * slots, width),
        vmem(n * slots, width),
        vmem(max(1, groups - 1), n * slots, width),
        vmem(n * slots, m * hidden),
        vmem(max(1, groups - 1), n * slots, 2 * hidden),
        vmem(n * slots, width),
        pltpu.SemaphoreType.DMA((16,)),
        pltpu.SemaphoreType.DMA((leaving,)),
        pltpu.SemaphoreType.DMA((signals,)),
    ]
    room = min(room[0], 60 * 2**20)
    arrays = (
        latent[0], jnp.transpose(rope_key[0]), latent_gain[None, :], tables, query_nope[0],
        query_rope[0], up_key, up_value, out_weight, residual[0], ffn_gain[None, :],
        jnp.transpose(routes, (0, 2, 1)), jnp.transpose(route_weight[0]),
        gate_weight[0], up_weight[0], down_weight[0],
    )
    middle, back, high, low = pl.pallas_call(
        functools.partial(layer_kernel, n, m, slots, parts),
        out_shape=(
            jax.ShapeDtypeStruct((tokens, width), BF16),
            jax.ShapeDtypeStruct((n * slots, width), BF16),
            jax.ShapeDtypeStruct((tokens, n * slots), BF16),
            jax.ShapeDtypeStruct((tokens, n * slots), BF16),
        ),
        in_specs=[HBM] * 16,
        out_specs=(VM,) * 4,
        scratch_shapes=scratch,
        compiler_params=pltpu.CompilerParams(
            collective_id=0, has_side_effects=True, vmem_limit_bytes=room
        ),
    )(*(pltpu.with_memory_space_constraint(x, pltpu.HBM) for x in arrays))
    chunks = max(1, width // 512)
    updated = pl.pallas_call(
        combine_kernel,
        out_shape=jax.ShapeDtypeStruct((tokens, width), BF16),
        in_specs=[VM] * 4,
        out_specs=HBM,
        scratch_shapes=[pltpu.VMEM((tokens, width), BF16), pltpu.SemaphoreType.DMA((chunks,))],
        compiler_params=pltpu.CompilerParams(vmem_limit_bytes=16 * 2**20),
    )(back, middle, high, low)
    return updated[None]


def solution(mesh):
    in_specs = (
        P("tp", "sp", None),
        P("tp", "sp", None),
        P("tp", "sp", None),
        P("tp", "sp", None),
        P("tp", "sp", None),
        P(),
        P(),
        P(),
        P(),
        P(),
        P(None, "sp", None),
        P("tp", "sp", None),
        P("sp", None, "tp"),
        P("sp", None, "tp"),
        P("sp", "tp", None),
    )
    out_specs = P("tp", "sp", None)
    return jax.shard_map(local, mesh=mesh, in_specs=in_specs, out_specs=out_specs, check_vma=False)
```
